32 devices in a mesh: fs: 4 (over z), tp: 4 (over y, x), rep: 2 (over core).
Axes of the slice: x: 2, y: 2, z: 4, core: 2. Of those that a mesh axis runs over, the one named last changes fastest.
Arguments:
- up_weight: float32 [2048, 8192], P('fs', ('tp', 'rep')), may hold values from -0.125 to 0.125
- up_momentum: float32 [2048, 8192], P('fs', ('tp', 'rep')), may hold values from -24 to 24
- up_grads: bfloat16 [2, 2048, 8192], P('rep', 'fs', 'tp'), may hold values from -2.09375 to 2.09375
- out_weight: float32 [2048, 2048], P('fs', ('tp', 'rep')), may hold values from -0.125 to 0.125
- out_momentum: float32 [2048, 2048], P('fs', ('tp', 'rep')), may hold values from -24 to 24
- out_grads: bfloat16 [2, 2048, 2048], P('rep', 'fs', 'tp'), may hold values from -2.09375 to 2.09375
Outputs:
- up_weight_new: float32 [2048, 8192], P('fs', ('tp', 'rep'))
- up_momentum_new: float32 [2048, 8192], P('fs', ('tp', 'rep'))
- up_direction: float32 [2048, 8192], P('fs', ('tp', 'rep'))
- out_weight_new: float32 [2048, 2048], P('fs', ('tp', 'rep'))
- out_momentum_new: float32 [2048, 2048], P('fs', ('tp', 'rep'))
- out_direction: float32 [2048, 2048], P('fs', ('tp', 'rep'))
The draws below stay inside these ranges and needn't reach their ends.
All inputs are finite; a program needn't handle non-finite values.
Results may differ from the reference program's by a relative error of at most 0.039.
Values may be sent and summed in bfloat16 or wider, within the bound.
A program may use at most 64 MiB of HBM per device.

```python
import math
import jax
import jax.numpy as jnp
from jax import lax

D = 2048
FF = 8192
DMIX = 2048
ITERS = 3
N_REP = 2


def spread_rows(key, row_count, width):
    keys = jax.random.split(key, 4)
    base = jax.random.normal(keys[0], (row_count, width), jnp.float32)
    base = jnp.clip(base, -5.5, 5.5)
    group_rows = row_count // 16
    group_scale = jnp.exp(jax.random.uniform(keys[1], (16,), jnp.float32, math.log(0.12), math.log(3.0)))
    row_scale = jnp.exp(jax.random.uniform(keys[2], (row_count,), jnp.float32, math.log(0.7), math.log(1.4)))
    scale = group_scale[jnp.arange(row_count) // group_rows] * row_scale
    return base * scale[:, None]


def draw_up_momentum(key, part):
    return spread_rows(jax.random.fold_in(key, 11), D, FF)


def draw_out_momentum(key, part):
    return spread_rows(jax.random.fold_in(key, 23), DMIX, D)


def level_of(stream_key, shape, pieces, least, top_value):
    def one(position, parts):
        steps = jax.random.uniform(jax.random.fold_in(jax.random.fold_in(stream_key, 6), position), (parts,), jnp.float32, least / len(pieces), top_value / len(pieces))
        return jnp.repeat(jnp.exp(steps), shape[position] // parts).reshape((-1,) + (1,) * (len(shape) - position - 1))

    loudness = one(*pieces[0])
    for cut in pieces[1:]:
        loudness = loudness * one(*cut)
    return loudness


def scatter_about(rng, extent, deviation, most, shards=(), kind=jnp.bfloat16):
    gain = level_of(rng, extent, shards, -0.22, 0.18) if shards else 1.0
    values = jax.random.normal(rng, extent, jnp.float32) * deviation * gain
    return jnp.minimum(jnp.maximum(values, -most), most).astype(kind)


def setup_inputs(seed: int = 0) -> dict:
    arg_keys = jax.random.split(jax.random.key(seed), 7)
    up_weight = scatter_about(arg_keys[0], (D, FF), D ** -0.5, 0.125, ((0, 4), (1, 8)), jnp.float32)
    up_momentum = draw_up_momentum(jax.random.fold_in(arg_keys[6], 71), 0)
    up_grads = scatter_about(arg_keys[2], (N_REP, D, FF), 0.35, 2.09375, ((0, 2), (1, 4), (2, 4)))
    out_weight = scatter_about(arg_keys[3], (DMIX, D), DMIX ** -0.5, 0.125, ((0, 4), (1, 8)), jnp.float32)
    out_momentum = draw_out_momentum(jax.random.fold_in(arg_keys[6], 71), 0)
    out_grads = scatter_about(arg_keys[5], (N_REP, DMIX, D), 0.35, 2.09375, ((0, 2), (1, 4), (2, 4)))
    return dict(up_weight=up_weight, up_momentum=up_momentum, up_grads=up_grads, out_weight=out_weight, out_momentum=out_momentum, out_grads=out_grads)


MOMENT = 0.9
RATE = 0.02
COEF_A = 3.4445
COEF_B = -4.775
COEF_C = 2.0315

def orthogonal(moment):
    current = moment
    for iteration in range(ITERS):
        values = current.astype(jnp.bfloat16)
        gram = jnp.dot(values, values.T, preferred_element_type=jnp.float32)
        if iteration == 0:
            square = 1.0 / (jnp.sqrt(jnp.sum(gram * gram)) + 1.0)
            factor = jnp.sqrt(square)
        else:
            square = 1.0
            factor = 1.0
        halved = (gram * square).astype(jnp.bfloat16)
        product = factor * jnp.dot(halved, values, preferred_element_type=jnp.float32)
        second = jnp.dot(halved, product.astype(jnp.bfloat16), preferred_element_type=jnp.float32)
        current = COEF_A * factor * current + COEF_B * product + COEF_C * second
    return current

def update(weight, momentum, grads):
    grad = lax.optimization_barrier(jnp.sum(grads.astype(jnp.float32), axis=0))
    moment = MOMENT * momentum + grad
    direction = orthogonal(moment) * math.sqrt(momentum.shape[1])
    return (weight - RATE * direction, moment, direction)

def reference(up_weight, up_momentum, up_grads, out_weight, out_momentum, out_grads):
    up_new, up_moment, up_step = update(up_weight, up_momentum, up_grads)
    out_new, out_moment, out_step = update(out_weight, out_momentum, out_grads)
    return (up_new, up_moment, up_step, out_new, out_moment, out_step)
```

```python
import math

import jax
import jax.numpy as jnp
from jax import lax
from jax.sharding import PartitionSpec as P

ITERS = 3
MOMENT = 0.9
RATE = 0.02
COEF_A = 3.4445
COEF_B = -4.775
COEF_C = 2.0315
BF = jnp.bfloat16
F32 = jnp.float32
ROLES = 2
CUTS = 8


def mm(a, b):
    return jnp.dot(a, b, preferred_element_type=F32)


def mm_t(a, b):
    return lax.dot_general(a, b, (((1,), (1,)), ((), ())), preferred_element_type=F32)


def reduced_grad(grads):
    size = lax.axis_size("rep")
    rows, cols = grads.shape
    pieces = grads.reshape(rows, size, cols // size).transpose(1, 0, 2)
    pieces = lax.all_to_all(pieces, "rep", split_axis=0, concat_axis=0, tiled=True)
    return jnp.sum(pieces.astype(F32), axis=0)


def to_columns(values):
    size = lax.axis_size("fs")
    rows, cols = values.shape
    pieces = values.reshape(rows, size, cols // size).transpose(1, 0, 2)
    pieces = lax.all_to_all(pieces, "fs", split_axis=0, concat_axis=0, tiled=True)
    return pieces.reshape(size * rows, cols // size)


def to_rows(values):
    size = lax.axis_size("fs")
    rows, cols = values.shape
    pieces = values.reshape(size, rows // size, cols)
    pieces = lax.all_to_all(pieces, "fs", split_axis=0, concat_axis=0, tiled=True)
    return pieces.transpose(1, 0, 2).reshape(rows // size, cols * size)


def swap_pairs(values):
    size = lax.axis_size("rep")
    return lax.ppermute(values, "rep", [(i, i ^ 1) for i in range(size)])


def pack_gram(x):
    step = x.shape[0] // CUTS
    rows = []
    for i in range(CUTS // 2):
        j = CUTS - 1 - i
        rows.append(
            jnp.concatenate(
                [
                    mm_t(x[i * step : (i + 1) * step], x[i * step :]).astype(BF),
                    mm_t(x[j * step : (j + 1) * step], x[j * step :]).astype(BF),
                ],
                axis=1,
            )
        )
    return jnp.concatenate(rows, axis=0)


def unpack_gram(packed):
    step = packed.shape[0] * 2 // CUTS
    upper = {}
    for i in range(CUTS // 2):
        row = packed[i * step : (i + 1) * step]
        upper[i] = row[:, : (CUTS - i) * step]
        upper[CUTS - 1 - i] = row[:, (CUTS - i) * step :]
    full = []
    for i in range(CUTS):
        left = [upper[j][:, (i - j) * step : (i - j + 1) * step].T for j in range(i)]
        full.append(jnp.concatenate(left + [upper[i]], axis=1))
    return jnp.concatenate(full, axis=0)


def next_gram(a):
    square = mm(a, a)
    q = (COEF_B * a.astype(F32) + COEF_C * square).astype(BF)
    w = (COEF_A * a.astype(F32) + mm(q, a)).astype(BF)
    return (COEF_A * w.astype(F32) + mm(q, w)).astype(BF)


def on_device(up_weight, up_momentum, up_grads, out_weight, out_momentum, out_grads):
    even = lax.axis_index("rep") % 2 == 0
    up_moment = MOMENT * up_momentum + reduced_grad(up_grads[0])
    out_moment = MOMENT * out_momentum + reduced_grad(out_grads[0])
    up = to_columns(up_moment.astype(BF))
    out = to_columns(out_moment.astype(BF))
    width, narrow = up.shape[1], out.shape[1]
    out = jnp.pad(out, ((0, 0), (0, width - narrow)))
    other = swap_pairs(jnp.where(even, out, up))
    values = jnp.concatenate([jnp.where(even, up, out), other], axis=1)
    gram = unpack_gram(lax.psum(pack_gram(values), ("fs", "tp"))) if lax.axis_size("rep") == 2 else None
    if gram is None:
        size = lax.axis_size("rep")
        groups = [[i for i in range(size) if i % 2 == k] for k in range(2)]
        packed = lax.psum(pack_gram(values), ("fs", "tp"))
        packed = lax.psum(packed, "rep", axis_index_groups=groups)
        gram = unpack_gram(packed)
    gram = gram.astype(F32)
    square = 1.0 / (jnp.sqrt(jnp.sum(gram * gram)) + 1.0)
    factor = jnp.sqrt(square)
    a = (gram * square).astype(BF)
    current = values.astype(F32)
    for iteration in range(ITERS):
        y = mm(a, current.astype(BF))
        if iteration == 0:
            y = factor * y
            current = factor * current
        z = mm(a, y.astype(BF))
        current = COEF_A * current + COEF_B * y + COEF_C * z
        if iteration < ITERS - 1:
            a = next_gram(a)
    final = current.astype(BF)
    mine, other = final[:, :width], swap_pairs(final[:, width:])
    up = to_rows(jnp.where(even, mine, other)).astype(F32)
    out = to_rows(jnp.where(even, other, mine)[:, :narrow]).astype(F32)
    group = lax.axis_size("tp") * lax.axis_size("rep")
    up_direction = up * math.sqrt(up_weight.shape[1] * group)
    out_direction = out * math.sqrt(out_weight.shape[1] * group)
    return (
        up_weight - RATE * up_direction,
        up_moment,
        up_direction,
        out_weight - RATE * out_direction,
        out_moment,
        out_direction,
    )


def solution(mesh):
    flat = P("fs", ("tp", "rep"))
    grads = P("rep", "fs", "tp")
    return jax.shard_map(
        on_device,
        mesh=mesh,
        in_specs=(flat, flat, grads, flat, flat, grads),
        out_specs=(flat,) * 6,
        check_vma=False,
    )
```
